512 devices in a mesh: sp: 128 (over z, x, core), tp: 4 (over y).
Axes of the slice: x: 4, y: 4, z: 16, core: 2. Of those that a mesh axis runs over, the one named last changes fastest.
Arguments:
- rows_in: bfloat16 [16384, 2048], P(('sp', 'tp')), may hold values from -8 to 8
- in_gain: float32 [2048], replicated, may hold values from 0.1 to 1.9
- query_down: bfloat16 [2048, 256], replicated, may hold values from -0.125 to 0.125
- query_gain: float32 [256], replicated, may hold values from 0.1 to 1.9
- kv_down: bfloat16 [2048, 128], replicated, may hold values from -0.125 to 0.125
- kv_gain: float32 [128], replicated, may hold values from 0.1 to 1.9
- rope_down: bfloat16 [2048, 64], replicated, may hold values from -0.125 to 0.125
- query_nope_up: bfloat16 [256, 512], P(None, 'tp'), may hold values from -0.375 to 0.375
- query_rope_up: bfloat16 [256, 256], P(None, 'tp'), may hold values from -0.375 to 0.375
- key_up: bfloat16 [128, 512], P(None, 'tp'), may hold values from -2.9811459 to 2.9811459
- value_up: bfloat16 [128, 512], P(None, 'tp'), may hold values from -0.5 to 0.5
- rec_query: bfloat16 [2048, 256], P(None, 'tp'), may hold values from -0.125 to 0.125
- rec_key: bfloat16 [2048, 256], P(None, 'tp'), may hold values from -0.125 to 0.125
- rec_value: bfloat16 [2048, 512], P(None, 'tp'), may hold values from -0.125 to 0.125
- gate_weight: bfloat16 [2048, 4, 4], P(None, None, 'tp'), may hold values from -0.125 to 0.125
- forget_level: float32 [16384, 2, 4], P('sp', None, 'tp'), may hold values from 0 to 14
- head_gain: float32 [512], P('tp'), may hold values from 0.1 to 1.9
- init_state: float32 [2, 4, 64, 128], P(None, 'tp'), may hold values from -384 to 384
- init_norm: float32 [2, 4, 64], P(None, 'tp'), may hold values from -384 to 384
- out_attn: bfloat16 [512, 2048], P('tp'), may hold values from -0.25 to 0.25
- out_rec: bfloat16 [512, 2048], P('tp'), may hold values from -0.25 to 0.25
Outputs:
- mixed_out: bfloat16 [16384, 2048], P(('sp', 'tp'))
The draws below stay inside these ranges and needn't reach their ends.
All inputs are finite; a program needn't handle non-finite values.
Results may differ from the reference program's by a relative error of at most 0.023.
Values may be sent and summed in bfloat16 or wider, within the bound.
A program may use at most 64 MiB of HBM per device.

```python
import math
import jax
import jax.numpy as jnp
from jax import lax

D = 2048
HA = 4
RECURRENT_HEADS = 4
QL = 256
KVL = 128
NOPE = 128
ROPE = 64
VH = 128
MK = 64
MV = 128
MBLOCK = 128
SEQUENCE_TOKENS = 16384
HAG = 1
HMG = 1
N_TP = 4


def draw_rows_in(key, part):
    key_noise = jax.random.fold_in(key, 11)
    key_means = jax.random.fold_in(key, 12)
    regions = 64
    region_of = jnp.arange(SEQUENCE_TOKENS) * regions // SEQUENCE_TOKENS
    noise = jax.random.normal(key_noise, (SEQUENCE_TOKENS, D), jnp.float32)
    centres = 0.7 * jax.random.normal(key_means, (regions, D), jnp.float32)
    values = jnp.clip(noise + centres[region_of], -8.0, 8.0)
    return values.astype(jnp.bfloat16)


def draw_key_up(key, part):
    key_base = jax.random.fold_in(key, 31)
    base = jnp.clip(jax.random.normal(key_base, (KVL, HA, NOPE), jnp.float32), -4.0, 4.0) * KVL ** (-0.5)
    return base.reshape(KVL, HA * NOPE).astype(jnp.bfloat16)


def draw_forget_level(key, part):
    key_slow = jax.random.fold_in(key, 21)
    key_shift = jax.random.fold_in(key, 22)
    key_spike = jax.random.fold_in(key, 23)
    slow_heads = jax.random.bernoulli(key_slow, 0.5, (2, RECURRENT_HEADS))
    floor_level_value = jnp.where(slow_heads, jnp.log(4.0 * SEQUENCE_TOKENS), jnp.log(80.0)).astype(jnp.float32)
    blocks = 256
    block_lookup = jnp.arange(SEQUENCE_TOKENS) * blocks // SEQUENCE_TOKENS
    offset_steps = jax.random.uniform(key_shift, (blocks, 2, RECURRENT_HEADS), jnp.float32, -0.7, 0.7)
    spike_position = jax.random.randint(key_spike, (2, 2, RECURRENT_HEADS), 0, SEQUENCE_TOKENS)
    spike_match = jnp.any(jnp.arange(SEQUENCE_TOKENS)[:, None, None, None] == spike_position[None], axis=1)
    level_value = jnp.where(spike_match, 0.8, floor_level_value[None] + offset_steps[block_lookup])
    return level_value.astype(jnp.float32)


def block_levels(key, dims, split, low, top_value):
    level = 1.0
    for dim, parts in split:
        draws = jax.random.uniform(jax.random.fold_in(jax.random.fold_in(key, 6), dim), (parts,), jnp.float32, low / len(split), top_value / len(split))
        level = level * jnp.repeat(jnp.exp(draws), dims[dim] // parts).reshape((-1,) + (1,) * (len(dims) - 1 - dim))
    return level


def gaussian(key, extent, spread, most, split=(), kind=jnp.bfloat16):
    level = block_levels(key, extent, split, -0.22, 0.18) if split else 1.0
    drawn = jax.random.normal(key, extent, jnp.float32) * spread * level
    return jnp.minimum(jnp.maximum(drawn, -most), most).astype(kind)


def setup_inputs(seed: int = 0) -> dict:
    splits = jax.random.split(jax.random.key(seed), 22)
    rows_in = draw_rows_in(jax.random.fold_in(splits[21], 71), 0)
    in_gain = jnp.clip(1.0 + 0.18 * jax.random.normal(splits[1], (D,), jnp.float32), 0.1, 1.9)
    query_down = gaussian(splits[2], (D, QL), D ** -0.5, 0.125)
    query_gain = jnp.clip(1.0 + 0.18 * jax.random.normal(splits[3], (QL,), jnp.float32), 0.1, 1.9)
    kv_down = gaussian(splits[4], (D, KVL), D ** -0.5, 0.125)
    kv_gain = jnp.clip(1.0 + 0.18 * jax.random.normal(splits[5], (KVL,), jnp.float32), 0.1, 1.9)
    rope_down = gaussian(splits[6], (D, ROPE), D ** -0.5, 0.125)
    query_nope_up = gaussian(splits[7], (QL, HA * NOPE), QL ** -0.5, 0.375, ((1, 4),))
    query_rope_up = gaussian(splits[8], (QL, HA * ROPE), QL ** -0.5, 0.375, ((1, 4),))
    key_up = draw_key_up(jax.random.fold_in(splits[21], 71), 0)
    value_up = gaussian(splits[10], (KVL, HA * VH), KVL ** -0.5, 0.5, ((1, 4),))
    rec_query = gaussian(splits[11], (D, RECURRENT_HEADS * MK), D ** -0.5, 0.125, ((1, 4),))
    rec_key = gaussian(splits[12], (D, RECURRENT_HEADS * MK), D ** -0.5, 0.125, ((1, 4),))
    rec_value = gaussian(splits[13], (D, RECURRENT_HEADS * MV), D ** -0.5, 0.125, ((1, 4),))
    gate_weight = gaussian(splits[14], (D, 4, RECURRENT_HEADS), D ** -0.5, 0.125, ((2, 4),))
    forget_level = draw_forget_level(jax.random.fold_in(splits[21], 71), 0)
    head_gain = jnp.clip(1.0 + 0.18 * jax.random.normal(splits[16], (RECURRENT_HEADS * MV,), jnp.float32), 0.1, 1.9)
    init_state = gaussian(splits[17], (2, RECURRENT_HEADS, MK, MV), (0.5 * SEQUENCE_TOKENS ** 0.5), 384.0, ((1, 4),), jnp.float32)
    init_norm = gaussian(splits[18], (2, RECURRENT_HEADS, MK), (0.5 * SEQUENCE_TOKENS ** 0.5), 384.0, ((1, 4),), jnp.float32)
    out_attn = gaussian(splits[19], (HA * VH, D), (HA * VH) ** -0.5, 0.25, ((0, 4),))
    out_rec = gaussian(splits[20], (RECURRENT_HEADS * MV, D), (RECURRENT_HEADS * MV) ** -0.5, 0.25, ((0, 4),))
    return dict(rows_in=rows_in, in_gain=in_gain, query_down=query_down, query_gain=query_gain, kv_down=kv_down, kv_gain=kv_gain, rope_down=rope_down, query_nope_up=query_nope_up, query_rope_up=query_rope_up, key_up=key_up, value_up=value_up, rec_query=rec_query, rec_key=rec_key, rec_value=rec_value, gate_weight=gate_weight, forget_level=forget_level, head_gain=head_gain, init_state=init_state, init_norm=init_norm, out_attn=out_attn, out_rec=out_rec)


EPS = 1e-06
NEG = -1e+30

def rms_rows(values, gains):
    return values * lax.rsqrt(lax.optimization_barrier(jnp.mean(values * values, axis=-1, keepdims=True)) + EPS) * gains.astype(jnp.float32)

def rotate(values, positions):
    half_len = values.shape[-1] // 2
    frequency = 10000.0 ** (-jnp.arange(half_len, dtype=jnp.float32) / half_len)
    angles = positions.astype(jnp.float32)[:, None] * frequency[None, :]
    angles = jnp.concatenate([angles, angles], axis=-1)[:, None, :]
    turned = jnp.concatenate([-values[..., half_len:], values[..., :half_len]], axis=-1)
    return values * jnp.cos(angles) + turned * jnp.sin(angles)

def recurrence(query, keys_in, value_in, log_in, log_keep, c_start, n_start, m_start, floor_value):
    head_count, seq_len = log_in.shape
    block_count = seq_len // MBLOCK
    lower_mask = jnp.tril(jnp.ones((MBLOCK, MBLOCK), bool))
    highest = lax.Precision.HIGHEST

    def to_blocks(array):
        return jnp.moveaxis(array.reshape((head_count, block_count, MBLOCK) + array.shape[2:]), 1, 0)

    def one_step(carried, inputs):
        c_state, n_state, m_state = carried
        q_block, k_block, v_block, in_block, keep_block = inputs
        log_cum = jnp.cumsum(keep_block, axis=-1)
        log_decay = jnp.where(lower_mask, log_cum[:, :, None] - log_cum[:, None, :] + in_block[:, None, :], NEG)
        carry_log = log_cum + m_state[:, None]
        row_max = jnp.maximum(lax.optimization_barrier(jnp.max(log_decay, axis=-1)), carry_log)
        gated = jnp.einsum('htd,hsd->hts', q_block, k_block, precision=highest) * jnp.exp(log_decay - row_max[..., None])
        carry_weight = jnp.exp(carry_log - row_max)
        numerator = jnp.einsum('hts,hse->hte', gated, v_block, precision=highest) + carry_weight[..., None] * jnp.einsum('htd,hde->hte', q_block, c_state, precision=highest)
        denominator = lax.optimization_barrier(jnp.sum(gated, axis=-1)) + carry_weight * jnp.einsum('htd,hd->ht', q_block, n_state, precision=highest)
        result = numerator / jnp.maximum(jnp.abs(denominator), floor_value * jnp.exp(-row_max))[..., None]
        cum_end = log_cum[:, -1]
        weight_log = cum_end[:, None] - log_cum + in_block
        new_max = jnp.maximum(cum_end + m_state, lax.optimization_barrier(jnp.max(weight_log, axis=-1)))
        decay_all = jnp.exp(cum_end + m_state - new_max)
        in_weights = jnp.exp(weight_log - new_max[:, None])
        c_state = decay_all[:, None, None] * c_state + jnp.einsum('hsd,hse->hde', k_block * in_weights[..., None], v_block, precision=highest)
        n_state = decay_all[:, None] * n_state + jnp.einsum('hs,hsd->hd', in_weights, k_block, precision=highest)
        return ((c_state, n_state, new_max), result)
    inputs = tuple((to_blocks(array) for array in (query, keys_in, value_in, log_in, log_keep)))
    _, outputs = lax.scan(one_step, (c_start, n_start, m_start), inputs)
    return jnp.moveaxis(outputs, 0, 1).reshape(head_count, seq_len, -1)

def heads_first(product, head_width):
    rounded = lax.optimization_barrier(product.astype(jnp.bfloat16))
    return rounded.astype(jnp.float32).reshape(product.shape[0], -1, head_width).transpose(1, 0, 2)

def reference(rows_in, in_gain, query_down, query_gain, kv_down, kv_gain, rope_down, query_nope_up, query_rope_up, key_up, value_up, rec_query, rec_key, rec_value, gate_weight, forget_level, head_gain, init_state, init_norm, out_attn, out_rec):
    f32 = jnp.float32
    bf16 = jnp.bfloat16
    positions = jnp.arange(SEQUENCE_TOKENS, dtype=jnp.int32)
    normed = rms_rows(rows_in.astype(f32), in_gain).astype(bf16)
    q_latent = rms_rows(jnp.dot(normed, query_down, preferred_element_type=f32), query_gain).astype(bf16)
    kv_latent = rms_rows(jnp.dot(normed, kv_down, preferred_element_type=f32), kv_gain).astype(bf16)
    key_rope = rotate(jnp.dot(normed, rope_down, preferred_element_type=f32)[:, None, :], positions)[:, 0, :].astype(bf16)
    query_nope = jnp.dot(q_latent, query_nope_up, preferred_element_type=f32).astype(bf16).reshape(SEQUENCE_TOKENS, HA, NOPE)
    query_rope = rotate(jnp.dot(q_latent, query_rope_up, preferred_element_type=f32).reshape(SEQUENCE_TOKENS, HA, ROPE), positions).astype(bf16)
    query_abs = jnp.einsum('thn,khn->thk', query_nope.astype(f32), key_up.astype(f32).reshape(KVL, HA, NOPE)).astype(bf16)
    queries = jnp.concatenate([query_abs, query_rope], axis=-1)
    key_rows = jnp.concatenate([kv_latent, key_rope], axis=-1)
    score_scale = (NOPE + ROPE) ** (-0.5)
    query_block = math.gcd(SEQUENCE_TOKENS, 128)

    def attend_block(block_q):
        rows_q = block_q.reshape(query_block * HA, KVL + ROPE)
        scores = jnp.dot(rows_q, key_rows.T, preferred_element_type=f32) * score_scale
        row_top = lax.optimization_barrier(jnp.max(scores, axis=-1, keepdims=True))
        expo_all = jnp.exp(scores - row_top)
        totals = lax.optimization_barrier(jnp.sum(expo_all, axis=-1, keepdims=True))
        latent = (jnp.dot(expo_all.astype(bf16), kv_latent, preferred_element_type=f32) / totals).astype(bf16)
        return latent.reshape(query_block, HA, KVL)
    attended = lax.map(attend_block, queries.reshape(SEQUENCE_TOKENS // query_block, query_block, HA, KVL + ROPE)).reshape(SEQUENCE_TOKENS, HA, KVL)
    attention_out = jnp.einsum('thk,khv->thv', attended.astype(f32), value_up.astype(f32).reshape(KVL, HA, VH)).astype(bf16).reshape(SEQUENCE_TOKENS, HA * VH)
    rec_q = heads_first(jnp.dot(normed, rec_query, preferred_element_type=f32), MK)
    rec_k = heads_first(jnp.dot(normed, rec_key, preferred_element_type=f32), MK) * MK ** (-0.5)
    rec_v = heads_first(jnp.dot(normed, rec_value, preferred_element_type=f32), MV)
    gate_pre = jnp.einsum('td,dgh->tgh', normed.astype(f32), gate_weight.astype(f32))
    input_fwd = gate_pre[:, 0].T
    keep_fwd = jax.nn.log_sigmoid(gate_pre[:, 1] + forget_level[:, 0]).T
    input_bwd = gate_pre[:, 2].T
    keep_bwd = jax.nn.log_sigmoid(gate_pre[:, 3] + forget_level[:, 1]).T
    zero_heads = jnp.zeros((RECURRENT_HEADS,), f32)
    floor_value = float(SEQUENCE_TOKENS) ** 0.5
    forward_h = recurrence(rec_q, rec_k, rec_v, input_fwd, keep_fwd, init_state[0], init_norm[0], zero_heads, floor_value)
    backward_h = recurrence(rec_q[:, ::-1], rec_k[:, ::-1], rec_v[:, ::-1], input_bwd[:, ::-1], keep_bwd[:, ::-1], init_state[1], init_norm[1], zero_heads, floor_value)[:, ::-1]
    summed = (forward_h + backward_h).transpose(1, 0, 2)
    recurrent_out = rms_rows(summed, head_gain.reshape(RECURRENT_HEADS, MV)).astype(bf16).reshape(SEQUENCE_TOKENS, RECURRENT_HEADS * MV)
    mixed_out = jnp.zeros((SEQUENCE_TOKENS, D), f32)
    for group in range(N_TP):
        att_cols = attention_out[:, group * HAG * VH:(group + 1) * HAG * VH]
        rec_cols = recurrent_out[:, group * HMG * MV:(group + 1) * HMG * MV]
        partial_value = jnp.dot(att_cols, out_attn[group * HAG * VH:(group + 1) * HAG * VH], preferred_element_type=f32)
        partial_value = partial_value + jnp.dot(rec_cols, out_rec[group * HMG * MV:(group + 1) * HMG * MV], preferred_element_type=f32)
        mixed_out = mixed_out + partial_value.astype(bf16).astype(f32)
    return mixed_out.astype(bf16)
```

```python
import functools
import math

import jax
import jax.numpy as jnp
import numpy as np
from jax import lax
from jax.experimental import pallas as pl
from jax.experimental.pallas import tpu as pltpu
from jax.sharding import Mesh
from jax.sharding import PartitionSpec as P

NOPE = 128
ROPE = 64
MK = 64
EPS = 1e-06
NEG = -1e30
MESH_ID = pl.DeviceIdType.MESH
SP = ("z", "x", "c")
SP_TP = ("z", "x", "c", "y")
F32 = jnp.float32
BF16 = jnp.bfloat16
HIGHEST = lax.Precision.HIGHEST


def nn(a, b, precision=None):
    return lax.dot_general(a, b, (((1,), (0,)), ((), ())), precision=precision, preferred_element_type=F32)


def nt(a, b):
    return lax.dot_general(a, b, (((1,), (1,)), ((), ())), preferred_element_type=F32)


def rms(values, gains):
    return values * lax.rsqrt(jnp.mean(values * values, axis=-1, keepdims=True) + EPS) * gains


def rotated(values, cos, sin):
    half = values.shape[-1] // 2
    turned = jnp.concatenate([-values[:, half:], values[:, :half]], axis=-1)
    return values * cos + turned * sin


def log_sigmoid(x):
    e = jnp.exp(-jnp.abs(x))
    log1p = jnp.where(e < 1e-3, e * (1.0 - e * (0.5 - e * (1.0 / 3.0))), jnp.log(1.0 + e))
    return jnp.minimum(x, 0.0) - log1p


def combine(early, late):
    c_e, n_e, m_e, f_e = early
    c_l, n_l, m_l, f_l = late
    peak = jnp.maximum(f_l + m_e, m_l)
    kept = jnp.exp(f_l + m_e - peak)
    fresh = jnp.exp(m_l - peak)
    return (kept * c_e + fresh * c_l, kept * n_e + fresh * n_l, peak, f_e + f_l)


def read_state(ref, at, lo, sr):
    tail = ref[at, lo + sr : lo + sr + 8, :]
    return (ref[at, lo : lo + sr, :], tail[0:1], tail[1:2], tail[2:3])


def write_state(ref, at, lo, sr, state):
    c, n, m, f = state
    ref[at, lo : lo + sr, :] = c
    ref[at, lo + sr : lo + sr + 8, :] = jnp.concatenate([n, m, f, jnp.zeros((5, 128), F32)], axis=0)


def rdma(src, dst, send, recv, where):
    return pltpu.make_async_remote_copy(
        src_ref=src, dst_ref=dst, send_sem=send, recv_sem=recv, device_id=where, device_id_type=MESH_ID
    )


def body(
    sizes,
    rows_ref, in_gain_ref, query_gain_ref, kv_gain_ref, gates_ref, forget_ref, head_gain_ref, init_c_ref, init_n_ref,
    block_tab_ref, row_tab_ref,
    qd_hbm, kvd_hbm, ropet_hbm, nope_hbm, rupt_hbm, kup_hbm, vup_hbm, rq_hbm, rk_hbm, rv_hbm, oa_hbm, or_hbm,
    out_ref,
    wqd, wkv, wrope, wnope, wrup, wkup, wvup, wt, wv, wout,
    nb, kb, qb, qa_s, qb_s, ss, mx, acc, lsum, acc2, sa, ra, pfx, tb, rb, sc, rc, po, pst, rp, rst, ob, ro,
    wsem, ny_s, ny_r, kz_s, kz_r, kx_s, kx_r, kc_s, kc_r, a_s, a_r, b_s, b_r, c_s, c_r, q_s, q_r, p_s, p_r, t_s, t_r, o_s, o_r,
):
    NZ, NX, NC, NY = sizes
    G = NX * NC
    SR = MK // G
    ST = SR + 8
    T = nb.shape[0]
    R = T // NY
    H = R // 2
    zi, xi, ci, yi = (lax.axis_index(a) for a in ("z", "x", "c", "y"))
    me = xi * NC + ci
    seq = NZ * NX * NC * T
    floor_value = float(seq) ** 0.5

    barrier = pltpu.get_barrier_semaphore()
    peers = 0
    for d in range(1, NY):
        pl.semaphore_signal(barrier, inc=1, device_id={"y": lax.rem(yi + d, NY)}, device_id_type=MESH_ID)
        peers += 1
    for d in range(1, NZ):
        pl.semaphore_signal(barrier, inc=1, device_id={"z": lax.rem(zi + d, NZ)}, device_id_type=MESH_ID)
        peers += 1
    for d in range(1, G):
        g = lax.rem(me + d, G)
        pl.semaphore_signal(barrier, inc=1, device_id={"x": g // NC, "c": lax.rem(g, NC)}, device_id_type=MESH_ID)
        peers += 1

    loads = [
        pltpu.make_async_copy(src, dst, wsem.at[i])
        for i, (src, dst) in enumerate(
            [
                (kvd_hbm, wkv), (ropet_hbm, wrope), (rk_hbm, wt.at[0:MK]), (rq_hbm, wt.at[MK : 2 * MK]), (rv_hbm, wv),
                (qd_hbm, wqd), (nope_hbm, wnope), (rupt_hbm, wrup), (kup_hbm, wkup), (vup_hbm, wvup),
                (oa_hbm, wout.at[0:128]), (or_hbm, wout.at[128:256]),
            ]
        )
    ]
    for c in loads:
        c.start()

    normed = rms(rows_ref[...].astype(F32), in_gain_ref[...]).astype(BF16)
    own_rows = pl.ds(pl.multiple_of(yi * R, R), R)
    nb[own_rows, :] = normed
    wt[2 * MK : 2 * MK + 16, :] = jnp.concatenate(
        [gates_ref[...], jnp.zeros((12, gates_ref.shape[1]), BF16)], axis=0
    )
    pl.semaphore_wait(barrier, peers)

    def to_y(d, src, dst, send, recv):
        return rdma(src, dst, send.at[d], recv.at[d], {"y": lax.rem(yi + d, NY)})

    ny = [to_y(d, nb.at[own_rows], nb.at[own_rows], ny_s, ny_r) for d in range(1, NY)]
    for c in ny:
        c.start()

    sp_index = (zi * NX + xi) * NC + ci
    block_row = block_tab_ref[pl.ds(sp_index, 1), :]
    cos_b, sin_b = block_row[:, :ROPE], block_row[:, ROPE:]

    def angles(table):
        cos_r, sin_r = table[:, :ROPE], table[:, ROPE:]
        return cos_b * cos_r - sin_b * sin_r, sin_b * cos_r + cos_b * sin_r

    loads[0].wait()
    loads[1].wait()
    latent = rms(nn(normed, wkv[...]), kv_gain_ref[...]).astype(BF16)
    rope = rotated(nt(normed, wrope[...]), *angles(row_tab_ref[own_rows, :])).astype(BF16)
    own_chunk = pl.ds(pl.multiple_of(zi * H, H), H)
    kb[me, own_chunk, :] = jnp.concatenate([latent[:H], rope[:H], rope[H:], latent[H:]], axis=1)

    def z_key(d, slot):
        rows = pl.ds(pl.multiple_of(slot * H, H), H)
        return rdma(
            kb.at[me, rows], kb.at[me, rows], kz_s.at[d], kz_r.at[d], {"z": lax.rem(zi + d, NZ)}
        )

    def start_z_key(d, _):
        z_key(d, zi).start()
        return 0

    lax.fori_loop(1, NZ, start_z_key, 0)

    for i in (2, 3, 4, 5):
        loads[i].wait()
    for d in range(1, NY):
        rows = pl.ds(pl.multiple_of(lax.rem(yi - d + NY, NY) * R, R), R)
        to_y(d, nb.at[rows], nb.at[rows], ny_s, ny_r).wait_recv()
    kqg = nt(wt[...], nb[...])
    v = nn(nb[...], wv[...]).astype(BF16)
    kq_t = jnp.transpose(kqg[0 : 2 * MK])
    k_t = kqg[0:MK].astype(BF16)
    kq = kq_t.astype(BF16)
    i_f = kqg[2 * MK : 2 * MK + 1]
    i_b = kqg[2 * MK + 2 : 2 * MK + 3]
    f_f = log_sigmoid(kqg[2 * MK + 1 : 2 * MK + 2] + forget_ref[0:1, :])
    f_b = log_sigmoid(kqg[2 * MK + 3 : 2 * MK + 4] + forget_ref[1:2, :])
    row_id = lax.broadcasted_iota(jnp.int32, (T, T), 0)
    col_id = lax.broadcasted_iota(jnp.int32, (T, T), 1)
    upto = row_id <= col_id
    after = row_id >= col_id
    logs = jnp.concatenate([f_f, f_b, jnp.zeros((6, T), F32)], axis=0)
    cum_f = nn(logs, upto.astype(F32), HIGHEST)[0:1]
    cum_b = nn(logs, after.astype(F32), HIGHEST)[1:2]
    cums = jnp.transpose(jnp.concatenate([cum_f, cum_b, jnp.zeros((6, T), F32)], axis=0))
    cum_f_col, cum_b_col = cums[:, 0:1], cums[:, 1:2]
    in_f, in_b = i_f - cum_f, i_b - cum_b
    end_f, end_b = cum_f[:, T - 1 : T], cum_b[:, 0:1]
    peak_f = jnp.max(end_f + in_f, axis=1, keepdims=True)
    peak_b = jnp.max(end_b + in_b, axis=1, keepdims=True)
    w_f = jnp.exp(end_f + in_f - peak_f)
    w_b = jnp.exp(end_b + in_b - peak_b)
    k_scaled = k_t.astype(F32) * (MK ** -0.5)
    weighted = jnp.concatenate([k_scaled * w_f, k_scaled * w_b], axis=0).astype(BF16)
    memory = nn(weighted, v)
    weights = jnp.concatenate([w_f, w_b, jnp.zeros((6, T), F32)], axis=0).astype(BF16)
    norms = nn(weights, kq) * (MK ** -0.5)
    spread = jnp.zeros((1, 128), F32)
    tail_f = (norms[0:1], peak_f + spread, end_f + spread)
    tail_b = (norms[1:2], peak_b + spread, end_b + spread)
    for g in range(G):
        write_state(sa, g, 0, SR, (memory[g * SR : (g + 1) * SR], *tail_f))
        write_state(sa, g, ST, SR, (memory[MK + g * SR : MK + (g + 1) * SR], *tail_b))

    def to_group(d, src, dst, send, recv):
        g = lax.rem(me + d, G)
        return rdma(src, dst, send.at[d], recv.at[d], {"x": g // NC, "c": lax.rem(g, NC)})

    stage_a = [to_group(d, sa.at[lax.rem(me + d, G)], ra.at[me], a_s, a_r) for d in range(1, G)]
    for c in stage_a:
        c.start()
    ra[me] = sa[me]

    for i in (6, 7, 8):
        loads[i].wait()
    q_latent = rms(nn(nb[...], wqd[...]), query_gain_ref[...]).astype(BF16)
    q_nope = nn(q_latent, wnope[...]).astype(BF16)
    q_abs = nt(q_nope, wkup[...]).astype(BF16)
    q_rope = rotated(nt(q_latent, wrup[...]), *angles(row_tab_ref[...])).astype(BF16)
    qb[yi] = jnp.concatenate([q_abs, q_rope, q_rope], axis=1)
    stage_q = [to_y(d, qb.at[yi], qb.at[yi], q_s, q_r) for d in range(1, NY)]
    for c in stage_q:
        c.start()

    def wait_z_key(d, _):
        z_key(d, lax.rem(zi - d + NZ, NZ)).wait_recv()
        return 0

    lax.fori_loop(1, NZ, wait_z_key, 0)

    def x_key(d, g):
        return rdma(kb.at[g], kb.at[g], kx_s.at[d], kx_r.at[d], {"x": lax.rem(xi + d, NX)})

    def c_key(d, g):
        return rdma(kb.at[g], kb.at[g], kc_s.at[d], kc_r.at[d], {"c": 1 - ci})

    stage_x = [x_key(d, me) for d in range(1, NX)]
    for c in stage_x:
        c.start()
    stage_k = [c_key(0, me)]
    stage_k[0].start()

    scores = nt(kq[:, MK : 2 * MK], kq[:, 0:MK]) * (MK ** -0.5)
    log_f = jnp.where(after, cum_f_col + in_f, NEG)
    log_b = jnp.where(upto, cum_b_col + in_b, NEG)
    max_f = jnp.max(log_f, axis=1, keepdims=True)
    max_b = jnp.max(log_b, axis=1, keepdims=True)
    gated_f = scores * jnp.exp(log_f - max_f)
    gated_b = scores * jnp.exp(log_b - max_b)
    num_f = nn(gated_f.astype(BF16), v)
    num_b = nn(gated_b.astype(BF16), v)
    den_f = jnp.sum(gated_f, axis=1, keepdims=True)
    den_b = jnp.sum(gated_b, axis=1, keepdims=True)

    for d in range(1, G):
        g = lax.rem(me - d + G, G)
        to_group(d, sa.at[me], ra.at[g], a_s, a_r).wait_recv()
    zero = (jnp.zeros((SR, 128), F32), spread, spread + NEG, spread)
    run = zero
    for g in range(G):
        write_state(pfx, g, 0, SR, run)
        run = combine(run, read_state(ra, g, 0, SR))
    write_state(tb, 0, 0, SR, run)
    run = zero
    for g in reversed(range(G)):
        write_state(pfx, g, ST, SR, run)
        run = combine(run, read_state(ra, g, ST, SR))
    write_state(tb, 1, 0, SR, run)

    def z_total(d, slot):
        return rdma(tb.at[(zi + d) // NZ], rb.at[slot], b_s.at[d], b_r.at[d], {"z": lax.rem(zi + d, NZ)})

    def start_z_total(d, _):
        z_total(d, zi).start()
        return 0

    lax.fori_loop(1, NZ, start_z_total, 0)

    for d in range(1, NY):
        slot = lax.rem(yi - d + NY, NY)
        to_y(d, qb.at[slot], qb.at[slot], q_s, q_r).wait_recv()
    lane = lax.broadcasted_iota(jnp.int32, (T, 128), 1)
    for h in range(NY):
        q_h = qb[h]
        rr = q_h[:, 128:256].astype(F32)
        first = jnp.where(lane < ROPE, rr, 0.0).astype(BF16)
        second = jnp.where(lane < ROPE, 0.0, rr).astype(BF16)
        qa_s[h * T : (h + 1) * T, :] = jnp.concatenate([q_h[:, 0:128], first], axis=1)
        qb_s[h * T : (h + 1) * T, :] = jnp.concatenate([second, q_h[:, 0:128]], axis=1)
    for d in range(1, NX):
        g = lax.rem(xi - d + NX, NX) * NC + ci
        x_key(d, g).wait_recv()
        stage_k.append(c_key(d, g))
        stage_k[-1].start()

    scale = (NOPE + ROPE) ** -0.5
    KEYS = kb.shape[1]

    def lane_max(s):
        parts = [s[:, i : i + 128] for i in range(0, s.shape[1], 128)]
        return functools.reduce(jnp.maximum, parts)

    def lane_sum(s):
        parts = [s[:, i : i + 128] for i in range(0, s.shape[1], 128)]
        return functools.reduce(jnp.add, parts)

    def share(core, total):
        mx[...] = jnp.full(mx.shape, NEG, F32)

        def look(i, _):
            g = i * NC + core
            s_a = nt(qa_s[...], kb[g, :, 0:256])
            ss[2 * i] = s_a
            s_b = nt(qb_s[...], kb[g, :, 128:384])
            ss[2 * i + 1] = s_b
            mx[...] = jnp.maximum(mx[...], jnp.maximum(lane_max(s_a), lane_max(s_b)))
            return 0

        lax.fori_loop(0, NX, look, 0)
        top = jnp.max(mx[...], axis=1, keepdims=True)
        total[...] = jnp.zeros(total.shape, F32)
        lsum[...] = jnp.zeros(lsum.shape, F32)

        def add(i, _):
            g = i * NC + core
            p_a = jnp.exp((ss[2 * i] - top) * scale)
            p_b = jnp.exp((ss[2 * i + 1] - top) * scale)
            lsum[...] += lane_sum(p_a) + lane_sum(p_b)
            total[...] += nn(p_a.astype(BF16), kb[g, :, 0:128]) + nn(p_b.astype(BF16), kb[g, :, 256:384])
            return 0

        lax.fori_loop(0, NX, add, 0)
        return top, jnp.sum(lsum[...], axis=1, keepdims=True)

    top_1, sum_1 = share(ci, acc)

    def wait_z_total(d, _):
        z_total(d, lax.rem(zi - d + NZ, NZ)).wait_recv()
        return 0

    lax.fori_loop(1, NZ, wait_z_total, 0)
    own_slice = pl.ds(pl.multiple_of(me * SR, SR), SR)
    pad = jnp.zeros((1, 128 - MK), F32)

    def initial(way):
        norm = jnp.concatenate([init_n_ref[way : way + 1, :], pad], axis=1)
        return (init_c_ref[way, own_slice, :], norm, spread, spread)

    run_f = lax.fori_loop(0, zi, lambda j, run: combine(run, read_state(rb, j, 0, SR)), initial(0))
    run_b = lax.fori_loop(
        0, NZ - 1 - zi, lambda j, run: combine(run, read_state(rb, NZ - 1 - j, 0, SR)), initial(1)
    )
    for g in range(G):
        write_state(sc, g, 0, SR, combine(run_f, read_state(pfx, g, 0, SR)))
        write_state(sc, g, ST, SR, combine(run_b, read_state(pfx, g, ST, SR)))
    stage_c = [to_group(d, sc.at[lax.rem(me + d, G)], rc.at[me], c_s, c_r) for d in range(1, G)]
    for c in stage_c:
        c.start()
    rc[me] = sc[me]

    for d in range(NX):
        g = lax.rem(xi - d + NX, NX) * NC + 1 - ci
        c_key(d, g).wait_recv()
    top_2, sum_2 = share(1 - ci, acc2)

    top = jnp.maximum(top_1, top_2)
    part_1 = jnp.exp((top_1 - top) * scale)
    part_2 = jnp.exp((top_2 - top) * scale)
    mass = part_1 * sum_1 + part_2 * sum_2
    partial = (part_1 * acc[...] + part_2 * acc2[...]) / mass
    log_mass = top * scale + jnp.log(mass)
    for h in range(NY):
        po[h] = partial[h * T : (h + 1) * T].astype(BF16)
        pst[h] = jnp.transpose(jnp.broadcast_to(log_mass[h * T : (h + 1) * T], (T, 128)))[0:8]
    stage_p = [to_y(d, po.at[lax.rem(yi + d, NY)], rp.at[yi], p_s, p_r) for d in range(1, NY)]
    stage_t = [to_y(d, pst.at[lax.rem(yi + d, NY)], rst.at[yi], t_s, t_r) for d in range(1, NY)]
    for c in stage_t + stage_p:
        c.start()
    rp[yi] = po[yi]
    rst[yi] = pst[yi]

    for d in range(1, G):
        g = lax.rem(me - d + G, G)
        to_group(d, sc.at[me], rc.at[g], c_s, c_r).wait_recv()
    state_f = jnp.concatenate([rc[g, 0:SR, :] for g in range(G)], axis=0)
    state_b = jnp.concatenate([rc[g, ST : ST + SR, :] for g in range(G)], axis=0)
    tail_f = rc[0, SR : SR + 8, :]
    tail_b = rc[0, ST + SR : ST + SR + 8, :]
    query = kq[:, MK : 2 * MK]
    carried = nn(query, jnp.concatenate([state_f, state_b], axis=1).astype(BF16))
    query32 = query.astype(F32)

    def finished(num, den, row_max, cum_col, from_state, tail):
        carry_log = cum_col + tail[1:2, 0:1]
        new_max = jnp.maximum(row_max, carry_log)
        inside = jnp.exp(row_max - new_max)
        outside = jnp.exp(carry_log - new_max)
        from_norm = jnp.sum(query32 * tail[0:1, 0:MK], axis=1, keepdims=True)
        below = inside * den + outside * from_norm
        above = inside * num + outside * from_state
        return above / jnp.maximum(jnp.abs(below), floor_value * jnp.exp(-new_max))

    both = finished(num_f, den_f, max_f, cum_f_col, carried[:, 0:128], tail_f) + finished(
        num_b, den_b, max_b, cum_b_col, carried[:, 128:256], tail_b
    )
    recurrent = rms(both, head_gain_ref[...]).astype(BF16)

    for d in range(1, NY):
        slot = lax.rem(yi - d + NY, NY)
        to_y(d, po.at[slot], rp.at[slot], p_s, p_r).wait_recv()
        to_y(d, pst.at[slot], rst.at[slot], t_s, t_r).wait_recv()
    cols = [jnp.transpose(rst[h])[:, 0:1] for h in range(NY)]
    top = functools.reduce(jnp.maximum, cols)
    parts = [jnp.exp(c - top) for c in cols]
    mass = functools.reduce(jnp.add, parts)
    merged = functools.reduce(jnp.add, [p * rp[h].astype(F32) for h, p in enumerate(parts)])
    attended = (merged / mass).astype(BF16)
    for i in (9, 10, 11):
        loads[i].wait()
    attention = nn(attended, wvup[...]).astype(BF16)
    joined = jnp.concatenate([attention, recurrent], axis=1)
    ob[...] = nn(joined, wout[...]).astype(BF16)

    def rows_of(y):
        return pl.ds(pl.multiple_of(y * R, R), R)

    stage_o = [to_y(d, ob.at[rows_of(lax.rem(yi + d, NY))], ro.at[yi], o_s, o_r) for d in range(1, NY)]
    for c in stage_o:
        c.start()
    result = ob[own_rows, :].astype(F32)
    for d in range(1, NY):
        slot = lax.rem(yi - d + NY, NY)
        to_y(d, ob.at[own_rows], ro.at[slot], o_s, o_r).wait_recv()
        result = result + ro[slot].astype(F32)
    out_ref[...] = result.astype(BF16)

    for c in ny + stage_a + stage_q + stage_x + stage_k + stage_c + stage_p + stage_t + stage_o:
        c.wait_send()

    def wait_z_sends(d, _):
        z_key(d, zi).wait_send()
        z_total(d, zi).wait_send()
        return 0

    lax.fori_loop(1, NZ, wait_z_sends, 0)


def rotary_tables(blocks, rows):
    half = ROPE // 2
    frequency = 10000.0 ** (-np.arange(half, dtype=np.float64) / half)

    def table(positions):
        angle = positions[:, None] * frequency[None, :]
        return np.concatenate([np.cos(angle), np.cos(angle), np.sin(angle), np.sin(angle)], axis=1).astype(np.float32)

    return table(np.arange(blocks, dtype=np.float64) * rows), table(np.arange(rows, dtype=np.float64))


def shards(
    sizes, rows_in, in_gain, query_down, query_gain, kv_down, kv_gain, rope_down, query_nope_up, query_rope_up, key_up,
    value_up, rec_query, rec_key, rec_value, gate_weight, forget_level, head_gain, init_state, init_norm, out_attn, out_rec,
):
    NZ, NX, NC, NY = sizes
    G = NX * NC
    SR = MK // G
    ST = SR + 8
    T = forget_level.shape[0]
    R, D = rows_in.shape
    H = R // 2
    KEYS = NZ * H
    block_tab, row_tab = rotary_tables(NZ * G, T)
    vmem_args = (
        rows_in, in_gain.reshape(1, -1), query_gain.reshape(1, -1), kv_gain.reshape(1, -1), gate_weight[:, :, 0].T,
        forget_level[:, :, 0].T, head_gain.reshape(1, -1), init_state[:, 0], init_norm[:, 0],
        jnp.asarray(block_tab), jnp.asarray(row_tab),
    )
    hbm_args = (
        query_down, kv_down, rope_down.T, query_nope_up, query_rope_up.T, key_up, value_up, rec_query.T, rec_key.T,
        rec_value, out_attn, out_rec,
    )
    dma = pltpu.SemaphoreType.DMA
    return pl.pallas_call(
        functools.partial(body, sizes),
        out_shape=jax.ShapeDtypeStruct((R, D), BF16),
        in_specs=[pl.BlockSpec(memory_space=pltpu.VMEM)] * len(vmem_args)
        + [pl.BlockSpec(memory_space=pltpu.HBM)] * len(hbm_args),
        out_specs=pl.BlockSpec(memory_space=pltpu.VMEM),
        scratch_shapes=[
            *[pltpu.VMEM(a.shape, BF16) for a in hbm_args[:7]],
            pltpu.VMEM((2 * MK + 16, D), BF16),
            pltpu.VMEM(rec_value.shape, BF16),
            pltpu.VMEM((256, D), BF16),
            pltpu.VMEM((T, D), BF16),
            pltpu.VMEM((G, KEYS, 384), BF16),
            pltpu.VMEM((NY, T, 256), BF16),
            pltpu.VMEM((NY * T, 256), BF16),
            pltpu.VMEM((NY * T, 256), BF16),
            pltpu.VMEM((2 * NX, NY * T, KEYS), F32),
            pltpu.VMEM((NY * T, 128), F32),
            pltpu.VMEM((NY * T, 128), F32),
            pltpu.VMEM((NY * T, 128), F32),
            pltpu.VMEM((NY * T, 128), F32),
            pltpu.VMEM((G, 2 * ST, 128), F32),
            pltpu.VMEM((G, 2 * ST, 128), F32),
            pltpu.VMEM((G, 2 * ST, 128), F32),
            pltpu.VMEM((2, ST, 128), F32),
            pltpu.VMEM((NZ, ST, 128), F32),
            pltpu.VMEM((G, 2 * ST, 128), F32),
            pltpu.VMEM((G, 2 * ST, 128), F32),
            pltpu.VMEM((NY, T, 128), BF16),
            pltpu.VMEM((NY, 8, T), F32),
            pltpu.VMEM((NY, T, 128), BF16),
            pltpu.VMEM((NY, 8, T), F32),
            pltpu.VMEM((T, D), BF16),
            pltpu.VMEM((NY, R, D), BF16),
            dma((12,)),
            *[dma((NY,))] * 2,
            *[dma((NZ,))] * 2,
            *[dma((NX,))] * 4,
            *[dma((G,))] * 2,
            *[dma((NZ,))] * 2,
            *[dma((G,))] * 2,
            *[dma((NY,))] * 8,
        ],
        compiler_params=pltpu.CompilerParams(
            collective_id=0, has_side_effects=True, vmem_limit_bytes=48 * 1024 * 1024
        ),
        name="layer",
    )(*vmem_args, *hbm_args)


def solution(mesh):
    sp, tp = mesh.shape["sp"], mesh.shape["tp"]
    sizes = (sp // 8, 4, 2, tp)
    split = Mesh(mesh.devices.reshape(sizes), SP_TP)
    in_specs = (
        P(SP_TP, None), P(), P(), P(), P(), P(), P(),
        P(None, "y"), P(None, "y"), P(None, "y"), P(None, "y"), P(None, "y"), P(None, "y"), P(None, "y"),
        P(None, None, "y"), P(SP, None, "y"), P("y"), P(None, "y", None, None), P(None, "y", None),
        P("y", None), P("y", None),
    )
    return jax.shard_map(
        functools.partial(shards, sizes), mesh=split, in_specs=in_specs, out_specs=P(SP_TP, None), check_vma=False
    )
```

```python
import functools
import math

import jax
import jax.numpy as jnp
import numpy as np
from jax import lax
from jax.experimental import pallas as pl
from jax.experimental.pallas import tpu as pltpu
from jax.sharding import Mesh
from jax.sharding import PartitionSpec as P

NOPE = 128
ROPE = 64
MK = 64
EPS = 1e-06
NEG = -1e30
MESH_ID = pl.DeviceIdType.MESH
SP = ("z", "x", "c")
SP_TP = ("z", "x", "c", "y")
F32 = jnp.float32
BF16 = jnp.bfloat16
HIGHEST = lax.Precision.HIGHEST


def nn(a, b, precision=None):
    return lax.dot_general(a, b, (((1,), (0,)), ((), ())), precision=precision, preferred_element_type=F32)


def nt(a, b):
    return lax.dot_general(a, b, (((1,), (1,)), ((), ())), preferred_element_type=F32)


def rms(values, gains):
    return values * lax.rsqrt(jnp.mean(values * values, axis=-1, keepdims=True) + EPS) * gains


def rotated(values, cos, sin):
    half = values.shape[-1] // 2
    turned = jnp.concatenate([-values[:, half:], values[:, :half]], axis=-1)
    return values * cos + turned * sin


def log_sigmoid(x):
    e = jnp.exp(-jnp.abs(x))
    log1p = jnp.where(e < 1e-3, e * (1.0 - e * (0.5 - e * (1.0 / 3.0))), jnp.log(1.0 + e))
    return jnp.minimum(x, 0.0) - log1p


def combine(early, late):
    c_e, n_e, m_e, f_e = early
    c_l, n_l, m_l, f_l = late
    peak = jnp.maximum(f_l + m_e, m_l)
    kept = jnp.exp(f_l + m_e - peak)
    fresh = jnp.exp(m_l - peak)
    return (kept * c_e + fresh * c_l, kept * n_e + fresh * n_l, peak, f_e + f_l)


def read_state(ref, at, lo, sr):
    tail = ref[at, lo + sr : lo + sr + 8, :]
    return (ref[at, lo : lo + sr, :], tail[0:1], tail[1:2], tail[2:3])


def write_state(ref, at, lo, sr, state):
    c, n, m, f = state
    ref[at, lo : lo + sr, :] = c
    ref[at, lo + sr : lo + sr + 8, :] = jnp.concatenate([n, m, f, jnp.zeros((5, 128), F32)], axis=0)


def rdma(src, dst, send, recv, where):
    return pltpu.make_async_remote_copy(
        src_ref=src, dst_ref=dst, send_sem=send, recv_sem=recv, device_id=where, device_id_type=MESH_ID
    )


def body(
    sizes,
    rows_hbm, in_gain_hbm, query_gain_hbm, kv_gain_hbm, gates_hbm, forget_hbm, head_gain_hbm, init_c_hbm, init_n_hbm,
    block_tab_hbm, row_tab_hbm,
    qd_hbm, kvd_hbm, ropet_hbm, nope_hbm, rupt_hbm, kup_hbm, vup_hbm, rq_hbm, rk_hbm, rv_hbm, oa_hbm, or_hbm,
    out_ref,
    rows_ref, in_gain_ref, query_gain_ref, kv_gain_ref, gates_ref, forget_ref, head_gain_ref, init_c_ref, init_n_ref,
    block_tab_ref, row_tab_ref,
    wqd, wkv, wrope, wnope, wrup, wkup, wvup, wt, wv, wout,
    nb, kb, qb, qa_s, qb_s, ss, mx, acc, lsum, acc2, sa, ra, pfx, tb, rb, sc, rc, po, pst, rp, rst, ob, ro,
    wsem, ny_s, ny_r, kz_s, kz_r, kx_s, kx_r, kc_s, kc_r, a_s, a_r, b_s, b_r, c_s, c_r, q_s, q_r, p_s, p_r, t_s, t_r, o_s, o_r,
):
    NZ, NX, NC, NY = sizes
    G = NX * NC
    SR = MK // G
    ST = SR + 8
    T = nb.shape[0]
    R = T // NY
    H = R // 2
    zi, xi, ci, yi = (lax.axis_index(a) for a in ("z", "x", "c", "y"))
    me = xi * NC + ci
    seq = NZ * NX * NC * T
    floor_value = float(seq) ** 0.5

    plan = (
        ("rows", rows_hbm, rows_ref), ("in_gain", in_gain_hbm, in_gain_ref), ("kv", kvd_hbm, wkv), ("rope", ropet_hbm, wrope),
        ("kv_gain", kv_gain_hbm, kv_gain_ref), ("blocks", block_tab_hbm, block_tab_ref), ("table", row_tab_hbm, row_tab_ref),
        ("gates", gates_hbm, gates_ref), ("rk", rk_hbm, wt.at[0:MK]), ("rq", rq_hbm, wt.at[MK : 2 * MK]),
        ("rv", rv_hbm, wv), ("forget", forget_hbm, forget_ref), ("qd", qd_hbm, wqd), ("q_gain", query_gain_hbm, query_gain_ref),
        ("nope", nope_hbm, wnope), ("rup", rupt_hbm, wrup), ("kup", kup_hbm, wkup), ("init_c", init_c_hbm, init_c_ref),
        ("init_n", init_n_hbm, init_n_ref), ("h_gain", head_gain_hbm, head_gain_ref), ("vup", vup_hbm, wvup),
        ("oa", oa_hbm, wout.at[0:128]), ("or", or_hbm, wout.at[128:256]),
    )
    loads = {name: pltpu.make_async_copy(src, dst, wsem.at[i]) for i, (name, src, dst) in enumerate(plan)}
    for c in loads.values():
        c.start()

    def ready(*names):
        for name in names:
            loads[name].wait()

    barrier = pltpu.get_barrier_semaphore()
    peers = 0
    for d in range(1, NY):
        pl.semaphore_signal(barrier, inc=1, device_id={"y": lax.rem(yi + d, NY)}, device_id_type=MESH_ID)
        peers += 1
    for d in range(1, NZ):
        pl.semaphore_signal(barrier, inc=1, device_id={"z": lax.rem(zi + d, NZ)}, device_id_type=MESH_ID)
        peers += 1
    for d in range(1, G):
        g = lax.rem(me + d, G)
        pl.semaphore_signal(barrier, inc=1, device_id={"x": g // NC, "c": lax.rem(g, NC)}, device_id_type=MESH_ID)
        peers += 1

    ready("rows", "in_gain")
    normed = rms(rows_ref[...].astype(F32), in_gain_ref[...]).astype(BF16)
    own_rows = pl.ds(pl.multiple_of(yi * R, R), R)
    nb[own_rows, :] = normed
    ready("gates")
    wt[2 * MK : 2 * MK + 16, :] = jnp.concatenate(
        [gates_ref[...], jnp.zeros((12, gates_ref.shape[1]), BF16)], axis=0
    )
    pl.semaphore_wait(barrier, peers)

    def to_y(d, src, dst, send, recv):
        return rdma(src, dst, send.at[d], recv.at[d], {"y": lax.rem(yi + d, NY)})

    ny = [to_y(d, nb.at[own_rows], nb.at[own_rows], ny_s, ny_r) for d in range(1, NY)]
    for c in ny:
        c.start()

    sp_index = (zi * NX + xi) * NC + ci
    ready("kv", "rope", "kv_gain", "blocks", "table")
    block_row = block_tab_ref[pl.ds(sp_index, 1), :]
    cos_b, sin_b = block_row[:, :ROPE], block_row[:, ROPE:]

    def angles(table):
        cos_r, sin_r = table[:, :ROPE], table[:, ROPE:]
        return cos_b * cos_r - sin_b * sin_r, sin_b * cos_r + cos_b * sin_r

    latent = rms(nn(normed, wkv[...]), kv_gain_ref[...]).astype(BF16)
    rope = rotated(nt(normed, wrope[...]), *angles(row_tab_ref[own_rows, :])).astype(BF16)
    own_chunk = pl.ds(pl.multiple_of(zi * H, H), H)
    kb[me, own_chunk, :] = jnp.concatenate([latent[:H], rope[:H], rope[H:], latent[H:]], axis=1)

    def z_key(d, slot):
        rows = pl.ds(pl.multiple_of(slot * H, H), H)
        return rdma(
            kb.at[me, rows], kb.at[me, rows], kz_s.at[d], kz_r.at[d], {"z": lax.rem(zi + d, NZ)}
        )

    def start_z_key(d, _):
        z_key(d, zi).start()
        return 0

    lax.fori_loop(1, NZ, start_z_key, 0)

    ready("rk", "rq", "rv", "forget")
    for d in range(1, NY):
        rows = pl.ds(pl.multiple_of(lax.rem(yi - d + NY, NY) * R, R), R)
        to_y(d, nb.at[rows], nb.at[rows], ny_s, ny_r).wait_recv()
    kqg = nt(wt[...], nb[...])
    v = nn(nb[...], wv[...]).astype(BF16)
    kq_t = jnp.transpose(kqg[0 : 2 * MK])
    k_t = kqg[0:MK].astype(BF16)
    kq = kq_t.astype(BF16)
    i_f = kqg[2 * MK : 2 * MK + 1]
    i_b = kqg[2 * MK + 2 : 2 * MK + 3]
    f_f = log_sigmoid(kqg[2 * MK + 1 : 2 * MK + 2] + forget_ref[0:1, :])
    f_b = log_sigmoid(kqg[2 * MK + 3 : 2 * MK + 4] + forget_ref[1:2, :])
    row_id = lax.broadcasted_iota(jnp.int32, (T, T), 0)
    col_id = lax.broadcasted_iota(jnp.int32, (T, T), 1)
    upto = row_id <= col_id
    after = row_id >= col_id
    logs = jnp.concatenate([f_f, f_b, jnp.zeros((6, T), F32)], axis=0)
    cum_f = nn(logs, upto.astype(F32), HIGHEST)[0:1]
    cum_b = nn(logs, after.astype(F32), HIGHEST)[1:2]
    cums = jnp.transpose(jnp.concatenate([cum_f, cum_b, jnp.zeros((6, T), F32)], axis=0))
    cum_f_col, cum_b_col = cums[:, 0:1], cums[:, 1:2]
    in_f, in_b = i_f - cum_f, i_b - cum_b
    end_f, end_b = cum_f[:, T - 1 : T], cum_b[:, 0:1]
    peak_f = jnp.max(end_f + in_f, axis=1, keepdims=True)
    peak_b = jnp.max(end_b + in_b, axis=1, keepdims=True)
    w_f = jnp.exp(end_f + in_f - peak_f)
    w_b = jnp.exp(end_b + in_b - peak_b)
    k_scaled = k_t.astype(F32) * (MK ** -0.5)
    weighted = jnp.concatenate([k_scaled * w_f, k_scaled * w_b], axis=0).astype(BF16)
    memory = nn(weighted, v)
    weights = jnp.concatenate([w_f, w_b, jnp.zeros((6, T), F32)], axis=0).astype(BF16)
    norms = nn(weights, kq) * (MK ** -0.5)
    spread = jnp.zeros((1, 128), F32)
    tail_f = (norms[0:1], peak_f + spread, end_f + spread)
    tail_b = (norms[1:2], peak_b + spread, end_b + spread)
    for g in range(G):
        write_state(sa, g, 0, SR, (memory[g * SR : (g + 1) * SR], *tail_f))
        write_state(sa, g, ST, SR, (memory[MK + g * SR : MK + (g + 1) * SR], *tail_b))

    def to_group(d, src, dst, send, recv):
        g = lax.rem(me + d, G)
        return rdma(src, dst, send.at[d], recv.at[d], {"x": g // NC, "c": lax.rem(g, NC)})

    stage_a = [to_group(d, sa.at[lax.rem(me + d, G)], ra.at[me], a_s, a_r) for d in range(1, G)]
    for c in stage_a:
        c.start()
    ra[me] = sa[me]

    ready("qd", "q_gain", "nope", "rup", "kup")
    q_latent = rms(nn(nb[...], wqd[...]), query_gain_ref[...]).astype(BF16)
    q_nope = nn(q_latent, wnope[...]).astype(BF16)
    q_abs = nt(q_nope, wkup[...]).astype(BF16)
    q_rope = rotated(nt(q_latent, wrup[...]), *angles(row_tab_ref[...])).astype(BF16)
    qb[yi] = jnp.concatenate([q_abs, q_rope, q_rope], axis=1)
    stage_q = [to_y(d, qb.at[yi], qb.at[yi], q_s, q_r) for d in range(1, NY)]
    for c in stage_q:
        c.start()

    def wait_z_key(d, _):
        z_key(d, lax.rem(zi - d + NZ, NZ)).wait_recv()
        return 0

    lax.fori_loop(1, NZ, wait_z_key, 0)

    def x_key(d, g):
        return rdma(kb.at[g], kb.at[g], kx_s.at[d], kx_r.at[d], {"x": lax.rem(xi + d, NX)})

    def c_key(d, g):
        return rdma(kb.at[g], kb.at[g], kc_s.at[d], kc_r.at[d], {"c": 1 - ci})

    stage_x = [x_key(d, me) for d in range(1, NX)]
    for c in stage_x:
        c.start()
    stage_k = [c_key(0, me)]
    stage_k[0].start()

    scores = nt(kq[:, MK : 2 * MK], kq[:, 0:MK]) * (MK ** -0.5)
    log_f = jnp.where(after, cum_f_col + in_f, NEG)
    log_b = jnp.where(upto, cum_b_col + in_b, NEG)
    max_f = jnp.max(log_f, axis=1, keepdims=True)
    max_b = jnp.max(log_b, axis=1, keepdims=True)
    gated_f = scores * jnp.exp(log_f - max_f)
    gated_b = scores * jnp.exp(log_b - max_b)
    num_f = nn(gated_f.astype(BF16), v)
    num_b = nn(gated_b.astype(BF16), v)
    den_f = jnp.sum(gated_f, axis=1, keepdims=True)
    den_b = jnp.sum(gated_b, axis=1, keepdims=True)

    for d in range(1, G):
        g = lax.rem(me - d + G, G)
        to_group(d, sa.at[me], ra.at[g], a_s, a_r).wait_recv()
    zero = (jnp.zeros((SR, 128), F32), spread, spread + NEG, spread)
    run = zero
    for g in range(G):
        write_state(pfx, g, 0, SR, run)
        run = combine(run, read_state(ra, g, 0, SR))
    write_state(tb, 0, 0, SR, run)
    run = zero
    for g in reversed(range(G)):
        write_state(pfx, g, ST, SR, run)
        run = combine(run, read_state(ra, g, ST, SR))
    write_state(tb, 1, 0, SR, run)

    def z_total(d, slot):
        return rdma(tb.at[(zi + d) // NZ], rb.at[slot], b_s.at[d], b_r.at[d], {"z": lax.rem(zi + d, NZ)})

    def start_z_total(d, _):
        z_total(d, zi).start()
        return 0

    lax.fori_loop(1, NZ, start_z_total, 0)

    for d in range(1, NY):
        slot = lax.rem(yi - d + NY, NY)
        to_y(d, qb.at[slot], qb.at[slot], q_s, q_r).wait_recv()
    lane = lax.broadcasted_iota(jnp.int32, (T, 128), 1)
    for h in range(NY):
        q_h = qb[h]
        rr = q_h[:, 128:256].astype(F32)
        first = jnp.where(lane < ROPE, rr, 0.0).astype(BF16)
        second = jnp.where(lane < ROPE, 0.0, rr).astype(BF16)
        qa_s[h * T : (h + 1) * T, :] = jnp.concatenate([q_h[:, 0:128], first], axis=1)
        qb_s[h * T : (h + 1) * T, :] = jnp.concatenate([second, q_h[:, 0:128]], axis=1)
    for d in range(1, NX):
        g = lax.rem(xi - d + NX, NX) * NC + ci
        x_key(d, g).wait_recv()
        stage_k.append(c_key(d, g))
        stage_k[-1].start()

    scale = (NOPE + ROPE) ** -0.5
    KEYS = kb.shape[1]

    def lane_max(s):
        parts = [s[:, i : i + 128] for i in range(0, s.shape[1], 128)]
        return functools.reduce(jnp.maximum, parts)

    def lane_sum(s):
        parts = [s[:, i : i + 128] for i in range(0, s.shape[1], 128)]
        return functools.reduce(jnp.add, parts)

    def share(core, total):
        mx[...] = jnp.full(mx.shape, NEG, F32)

        def look(i, _):
            g = i * NC + core
            s_a = nt(qa_s[...], kb[g, :, 0:256])
            ss[2 * i] = s_a
            s_b = nt(qb_s[...], kb[g, :, 128:384])
            ss[2 * i + 1] = s_b
            mx[...] = jnp.maximum(mx[...], jnp.maximum(lane_max(s_a), lane_max(s_b)))
            return 0

        lax.fori_loop(0, NX, look, 0)
        top = jnp.max(mx[...], axis=1, keepdims=True)
        total[...] = jnp.zeros(total.shape, F32)
        lsum[...] = jnp.zeros(lsum.shape, F32)

        def add(i, _):
            g = i * NC + core
            p_a = jnp.exp((ss[2 * i] - top) * scale)
            p_b = jnp.exp((ss[2 * i + 1] - top) * scale)
            lsum[...] += lane_sum(p_a) + lane_sum(p_b)
            total[...] += nn(p_a.astype(BF16), kb[g, :, 0:128]) + nn(p_b.astype(BF16), kb[g, :, 256:384])
            return 0

        lax.fori_loop(0, NX, add, 0)
        return top, jnp.sum(lsum[...], axis=1, keepdims=True)

    top_1, sum_1 = share(ci, acc)

    def wait_z_total(d, _):
        z_total(d, lax.rem(zi - d + NZ, NZ)).wait_recv()
        return 0

    lax.fori_loop(1, NZ, wait_z_total, 0)
    ready("init_c", "init_n", "h_gain")
    own_slice = pl.ds(pl.multiple_of(me * SR, SR), SR)
    pad = jnp.zeros((1, 128 - MK), F32)

    def initial(way):
        norm = jnp.concatenate([init_n_ref[way : way + 1, :], pad], axis=1)
        return (init_c_ref[way, own_slice, :], norm, spread, spread)

    run_f = lax.fori_loop(0, zi, lambda j, run: combine(run, read_state(rb, j, 0, SR)), initial(0))
    run_b = lax.fori_loop(
        0, NZ - 1 - zi, lambda j, run: combine(run, read_state(rb, NZ - 1 - j, 0, SR)), initial(1)
    )
    for g in range(G):
        write_state(sc, g, 0, SR, combine(run_f, read_state(pfx, g, 0, SR)))
        write_state(sc, g, ST, SR, combine(run_b, read_state(pfx, g, ST, SR)))
    stage_c = [to_group(d, sc.at[lax.rem(me + d, G)], rc.at[me], c_s, c_r) for d in range(1, G)]
    for c in stage_c:
        c.start()
    rc[me] = sc[me]

    for d in range(NX):
        g = lax.rem(xi - d + NX, NX) * NC + 1 - ci
        c_key(d, g).wait_recv()
    top_2, sum_2 = share(1 - ci, acc2)

    top = jnp.maximum(top_1, top_2)
    part_1 = jnp.exp((top_1 - top) * scale)
    part_2 = jnp.exp((top_2 - top) * scale)
    mass = part_1 * sum_1 + part_2 * sum_2
    partial = (part_1 * acc[...] + part_2 * acc2[...]) / mass
    log_mass = top * scale + jnp.log(mass)
    for h in range(NY):
        po[h] = partial[h * T : (h + 1) * T].astype(BF16)
        pst[h] = jnp.transpose(jnp.broadcast_to(log_mass[h * T : (h + 1) * T], (T, 128)))[0:8]
    stage_p = [to_y(d, po.at[lax.rem(yi + d, NY)], rp.at[yi], p_s, p_r) for d in range(1, NY)]
    stage_t = [to_y(d, pst.at[lax.rem(yi + d, NY)], rst.at[yi], t_s, t_r) for d in range(1, NY)]
    for c in stage_t + stage_p:
        c.start()
    rp[yi] = po[yi]
    rst[yi] = pst[yi]

    for d in range(1, G):
        g = lax.rem(me - d + G, G)
        to_group(d, sc.at[me], rc.at[g], c_s, c_r).wait_recv()
    state_f = jnp.concatenate([rc[g, 0:SR, :] for g in range(G)], axis=0)
    state_b = jnp.concatenate([rc[g, ST : ST + SR, :] for g in range(G)], axis=0)
    tail_f = rc[0, SR : SR + 8, :]
    tail_b = rc[0, ST + SR : ST + SR + 8, :]
    query = kq[:, MK : 2 * MK]
    carried = nn(query, jnp.concatenate([state_f, state_b], axis=1).astype(BF16))
    query32 = query.astype(F32)

    def finished(num, den, row_max, cum_col, from_state, tail):
        carry_log = cum_col + tail[1:2, 0:1]
        new_max = jnp.maximum(row_max, carry_log)
        inside = jnp.exp(row_max - new_max)
        outside = jnp.exp(carry_log - new_max)
        from_norm = jnp.sum(query32 * tail[0:1, 0:MK], axis=1, keepdims=True)
        below = inside * den + outside * from_norm
        above = inside * num + outside * from_state
        return above / jnp.maximum(jnp.abs(below), floor_value * jnp.exp(-new_max))

    both = finished(num_f, den_f, max_f, cum_f_col, carried[:, 0:128], tail_f) + finished(
        num_b, den_b, max_b, cum_b_col, carried[:, 128:256], tail_b
    )
    recurrent = rms(both, head_gain_ref[...]).astype(BF16)

    for d in range(1, NY):
        slot = lax.rem(yi - d + NY, NY)
        to_y(d, po.at[slot], rp.at[slot], p_s, p_r).wait_recv()
        to_y(d, pst.at[slot], rst.at[slot], t_s, t_r).wait_recv()
    cols = [jnp.transpose(rst[h])[:, 0:1] for h in range(NY)]
    top = functools.reduce(jnp.maximum, cols)
    parts = [jnp.exp(c - top) for c in cols]
    mass = functools.reduce(jnp.add, parts)
    merged = functools.reduce(jnp.add, [p * rp[h].astype(F32) for h, p in enumerate(parts)])
    attended = (merged / mass).astype(BF16)
    ready("vup", "oa", "or")
    attention = nn(attended, wvup[...]).astype(BF16)
    joined = jnp.concatenate([attention, recurrent], axis=1)
    ob[...] = nn(joined, wout[...]).astype(BF16)

    def rows_of(y):
        return pl.ds(pl.multiple_of(y * R, R), R)

    stage_o = [to_y(d, ob.at[rows_of(lax.rem(yi + d, NY))], ro.at[yi], o_s, o_r) for d in range(1, NY)]
    for c in stage_o:
        c.start()
    result = ob[own_rows, :].astype(F32)
    for d in range(1, NY):
        slot = lax.rem(yi - d + NY, NY)
        to_y(d, ob.at[own_rows], ro.at[slot], o_s, o_r).wait_recv()
        result = result + ro[slot].astype(F32)
    out_ref[...] = result.astype(BF16)

    for c in ny + stage_a + stage_q + stage_x + stage_k + stage_c + stage_p + stage_t + stage_o:
        c.wait_send()

    def wait_z_sends(d, _):
        z_key(d, zi).wait_send()
        z_total(d, zi).wait_send()
        return 0

    lax.fori_loop(1, NZ, wait_z_sends, 0)


def rotary_tables(blocks, rows):
    half = ROPE // 2
    frequency = 10000.0 ** (-np.arange(half, dtype=np.float64) / half)

    def table(positions):
        angle = positions[:, None] * frequency[None, :]
        return np.concatenate([np.cos(angle), np.cos(angle), np.sin(angle), np.sin(angle)], axis=1).astype(np.float32)

    return table(np.arange(blocks, dtype=np.float64) * rows), table(np.arange(rows, dtype=np.float64))


def shards(
    sizes, rows_in, in_gain, query_down, query_gain, kv_down, kv_gain, rope_down, query_nope_up, query_rope_up, key_up,
    value_up, rec_query, rec_key, rec_value, gate_weight, forget_level, head_gain, init_state, init_norm, out_attn, out_rec,
):
    NZ, NX, NC, NY = sizes
    G = NX * NC
    SR = MK // G
    ST = SR + 8
    T = forget_level.shape[0]
    R, D = rows_in.shape
    H = R // 2
    KEYS = NZ * H
    block_tab, row_tab = rotary_tables(NZ * G, T)
    small_args = (
        rows_in, in_gain.reshape(1, -1), query_gain.reshape(1, -1), kv_gain.reshape(1, -1), gate_weight[:, :, 0].T,
        forget_level[:, :, 0].T, head_gain.reshape(1, -1), init_state[:, 0], init_norm[:, 0],
        jnp.asarray(block_tab), jnp.asarray(row_tab),
    )
    hbm_args = (
        query_down, kv_down, rope_down.T, query_nope_up, query_rope_up.T, key_up, value_up, rec_query.T, rec_key.T,
        rec_value, out_attn, out_rec,
    )
    dma = pltpu.SemaphoreType.DMA
    return pl.pallas_call(
        functools.partial(body, sizes),
        out_shape=jax.ShapeDtypeStruct((R, D), BF16),
        in_specs=[pl.BlockSpec(memory_space=pltpu.HBM)] * (len(small_args) + len(hbm_args)),
        out_specs=pl.BlockSpec(memory_space=pltpu.VMEM),
        scratch_shapes=[
            *[pltpu.VMEM(a.shape, a.dtype) for a in (*small_args, *hbm_args[:7])],
            pltpu.VMEM((2 * MK + 16, D), BF16),
            pltpu.VMEM(rec_value.shape, BF16),
            pltpu.VMEM((256, D), BF16),
            pltpu.VMEM((T, D), BF16),
            pltpu.VMEM((G, KEYS, 384), BF16),
            pltpu.VMEM((NY, T, 256), BF16),
            pltpu.VMEM((NY * T, 256), BF16),
            pltpu.VMEM((NY * T, 256), BF16),
            pltpu.VMEM((2 * NX, NY * T, KEYS), F32),
            pltpu.VMEM((NY * T, 128), F32),
            pltpu.VMEM((NY * T, 128), F32),
            pltpu.VMEM((NY * T, 128), F32),
            pltpu.VMEM((NY * T, 128), F32),
            pltpu.VMEM((G, 2 * ST, 128), F32),
            pltpu.VMEM((G, 2 * ST, 128), F32),
            pltpu.VMEM((G, 2 * ST, 128), F32),
            pltpu.VMEM((2, ST, 128), F32),
            pltpu.VMEM((NZ, ST, 128), F32),
            pltpu.VMEM((G, 2 * ST, 128), F32),
            pltpu.VMEM((G, 2 * ST, 128), F32),
            pltpu.VMEM((NY, T, 128), BF16),
            pltpu.VMEM((NY, 8, T), F32),
            pltpu.VMEM((NY, T, 128), BF16),
            pltpu.VMEM((NY, 8, T), F32),
            pltpu.VMEM((T, D), BF16),
            pltpu.VMEM((NY, R, D), BF16),
            dma((23,)),
            *[dma((NY,))] * 2,
            *[dma((NZ,))] * 2,
            *[dma((NX,))] * 4,
            *[dma((G,))] * 2,
            *[dma((NZ,))] * 2,
            *[dma((G,))] * 2,
            *[dma((NY,))] * 8,
        ],
        compiler_params=pltpu.CompilerParams(
            collective_id=0, has_side_effects=True, vmem_limit_bytes=62 * 1024 * 1024
        ),
        name="layer",
    )(*small_args, *hbm_args)


def solution(mesh):
    sp, tp = mesh.shape["sp"], mesh.shape["tp"]
    sizes = (sp // 8, 4, 2, tp)
    split = Mesh(mesh.devices.reshape(sizes), SP_TP)
    in_specs = (
        P(SP_TP, None), P(), P(), P(), P(), P(), P(),
        P(None, "y"), P(None, "y"), P(None, "y"), P(None, "y"), P(None, "y"), P(None, "y"), P(None, "y"),
        P(None, None, "y"), P(SP, None, "y"), P("y"), P(None, "y", None, None), P(None, "y", None),
        P("y", None), P("y", None),
    )
    return jax.shard_map(
        functools.partial(shards, sizes), mesh=split, in_specs=in_specs, out_specs=P(SP_TP, None), check_vma=False
    )
```
